32 devices in a mesh: sp: 8 (over z, y), tp: 4 (over x, core).
Axes of the slice: x: 2, y: 2, z: 4, core: 2. Of those that a mesh axis runs over, the one named last changes fastest.
Arguments:
- resid: bfloat16 [8192, 2048], P(('sp', 'tp')), may hold values from -6 to 6
- queries: bfloat16 [8192, 2048], P('sp', 'tp'), may hold values from -6 to 6
- keys: bfloat16 [8192, 2048], P('sp', 'tp'), may hold values from -6 to 6
- values: bfloat16 [8192, 4096], P('sp', 'tp'), may hold values from -6 to 6
- gates: bfloat16 [8192, 4096], P('sp', 'tp'), may hold values from -6 to 6
- log_decay: float32 [8, 8192], P('tp', 'sp'), may hold values from -1 to 0
- retention_output_weight: bfloat16 [4096, 2048], P('tp'), may hold values from -0.125 to 0.125
- norm_gain: bfloat16 [2048], replicated, may hold values from 0.099609375 to 1.8984375
- up_weight: bfloat16 [2048, 8192], P('sp', 'tp'), may hold values from -0.125 to 0.125
- down_weight: bfloat16 [8192, 2048], P('tp', 'sp'), may hold values from -0.0625 to 0.0625
Outputs:
- layer_out: bfloat16 [8192, 2048], P(('sp', 'tp'))
The draws below stay inside these ranges and needn't reach their ends.
All inputs are finite; a program needn't handle non-finite values.
Results may differ from the reference program's by a relative error of at most 0.02.
Values may be sent and summed in bfloat16 or wider, within the bound.
A program may use at most 128 MiB of HBM per device.

```python
import math
import jax
import jax.numpy as jnp
from jax import lax

D = 2048
HEADS = 8
DK = 256
DV = 512
FF = 8192
BLOCK = 128
TOK_DEV = 1024
SEQ = 8192
N_TP = 4


def draw_log_decay(key, part):
    key_sequence_order, key_reach, key_block, key_jitter, key_place, key_keep = jax.random.split(jax.random.fold_in(key, 7), 6)
    order = jax.random.permutation(key_sequence_order, HEADS)
    fast = order < HEADS // 2
    reach = jnp.exp(jax.random.uniform(key_reach, (HEADS,), jnp.float32, math.log(30.0), math.log(100.0)))
    fast_rate = -math.log(10.0) / reach
    slow_rate = jnp.full((HEADS,), -0.1 * math.log(10.0) / SEQ, jnp.float32)
    rate = jnp.where(fast, fast_rate, slow_rate)
    segments = SEQ // TOK_DEV
    factor = jnp.exp(jax.random.uniform(key_block, (HEADS, segments, 1), jnp.float32, math.log(0.5), math.log(2.0)))
    jitter = jnp.exp(jax.random.uniform(key_jitter, (HEADS, segments, TOK_DEV), jnp.float32, -0.5, 0.5))
    per_token_slot = (rate[:, None, None] * factor * jitter).reshape(HEADS, SEQ)
    places = jax.random.randint(key_place, (HEADS, 2), 0, SEQ)
    surviving_items = jax.random.uniform(key_keep, (HEADS, 2), jnp.float32, 0.5, 0.8)
    agreement_count = jnp.arange(SEQ)[None, None, :] == places[:, :, None]
    cluster_bundles = jnp.sum(jnp.where(agreement_count, jnp.log(surviving_items)[:, :, None], 0.0), axis=1)
    return (per_token_slot + cluster_bundles).astype(jnp.float32)


def block_scale(key, dims, cuts, smallest, top_value):
    loudness, own = 1.0, jax.random.fold_in(key, 6)
    for dim, blocks in cuts:
        draws = jnp.exp(jax.random.uniform(jax.random.fold_in(own, dim), (blocks,), jnp.float32, smallest / len(cuts), top_value / len(cuts)))
        loudness = loudness * jnp.repeat(draws, dims[dim] // blocks).reshape([-1 if axis == dim else 1 for axis in range(len(dims))])
    return loudness


def normal_values(rng, dims, scale, limit, pieces=(), held_as=jnp.bfloat16):
    array = scale * jax.random.normal(rng, dims, jnp.float32)
    if pieces:
        array = array * block_scale(rng, dims, pieces, -0.22, 0.18)
    return jnp.clip(array, -limit, limit).astype(held_as)


def setup_inputs(seed: int = 0) -> dict:
    arg_keys = jax.random.split(jax.random.key(seed), 11)
    return {
        "resid": normal_values(arg_keys[0], (SEQ, D), 1.0, 6.0, ((0, 32),)),
        "queries": normal_values(arg_keys[1], (SEQ, HEADS * DK), 1.0, 6.0, ((0, 8), (1, 4))),
        "keys": normal_values(arg_keys[2], (SEQ, HEADS * DK), 1.0, 6.0, ((0, 8), (1, 4))),
        "values": normal_values(arg_keys[3], (SEQ, HEADS * DV), 1.0, 6.0, ((0, 8), (1, 4))),
        "gates": normal_values(arg_keys[4], (SEQ, HEADS * DV), 1.0, 6.0, ((0, 8), (1, 4))),
        "log_decay": draw_log_decay(jax.random.fold_in(arg_keys[10], 71), 0),
        "retention_output_weight": normal_values(arg_keys[6], (HEADS * DV, D), (HEADS * DV // 2) ** -0.5, 0.125, ((0, 4),)),
        "norm_gain": jnp.clip(1.0 + 0.18 * jax.random.normal(arg_keys[7], (D,), jnp.float32), 0.099609375, 1.8984375).astype(jnp.bfloat16),
        "up_weight": normal_values(arg_keys[8], (D, FF), D ** -0.5, 0.125, ((0, 8), (1, 4))),
        "down_weight": normal_values(arg_keys[9], (FF, D), FF ** -0.5, 0.0625, ((0, 4), (1, 8))),
    }


tiny_stabilizer = 1e-06

def round_trip(values_in):
    return lax.optimization_barrier(values_in.astype(jnp.bfloat16)).astype(jnp.float32)

def rotate(values_in, token_indices):
    half_width = values_in.shape[-1] // 2
    inverse = 10000.0 ** (-jnp.arange(0, 2 * half_width, 2, dtype=jnp.float32) / (2 * half_width))
    angles = token_indices[:, None].astype(jnp.float32) * inverse[None, :]
    cosine = jnp.cos(angles)[:, None, :]
    sine_lookup = jnp.sin(angles)[:, None, :]
    first_half = values_in[..., :half_width]
    second = values_in[..., half_width:]
    return jnp.concatenate([first_half * cosine - second * sine_lookup, first_half * sine_lookup + second * cosine], axis=-1)

def normalize(updated, norm_gain):
    widened = updated.astype(jnp.float32)
    scaled = widened * lax.rsqrt(lax.optimization_barrier(jnp.mean(widened * widened, axis=-1, keepdims=True)) + tiny_stabilizer)
    return (scaled * norm_gain.astype(jnp.float32)).astype(jnp.bfloat16)

def block_step(carry_state, per_block):
    query_blk, key_blk, value_blk, gate_blk, cum_blk = per_block
    length = cum_blk.shape[1]
    causal = jnp.arange(length)[:, None] >= jnp.arange(length)[None, :]
    spread = cum_blk[:, :, None] - cum_blk[:, None, :]
    factor = jnp.where(causal[None], jnp.exp(jnp.minimum(spread, 0.0)), 0.0)
    scores = jnp.einsum('ihd,jhd->hij', query_blk, key_blk)
    weights = round_trip(scores * factor)
    within_block = jnp.einsum('hij,jhv->ihv', weights, value_blk)
    decayed = round_trip(query_blk * jnp.exp(cum_blk).T[:, :, None])
    carried_part = jnp.einsum('ihd,hdv->ihv', decayed, round_trip(carry_state))
    retained = within_block + carried_part
    normed = retained * lax.rsqrt(lax.optimization_barrier(jnp.mean(retained * retained, axis=-1, keepdims=True)) + tiny_stabilizer)
    gated_out = (jax.nn.silu(gate_blk) * normed).astype(jnp.bfloat16)
    tile_count_all = cum_blk[:, -1]
    key_decayed = round_trip(key_blk * jnp.exp(tile_count_all[:, None] - cum_blk).T[:, :, None])
    update = jnp.einsum('jhd,jhv->hdv', key_decayed, value_blk)
    return (jnp.exp(tile_count_all)[:, None, None] * carry_state + update, gated_out)

def grouped_product(left, right, groups):
    group_width = left.shape[1] // groups

    def add_group(running, number):
        first_row = (number * group_width).astype(jnp.int32)
        left_part = lax.dynamic_slice_in_dim(left, first_row, group_width, 1)
        right_part = lax.dynamic_slice_in_dim(right, first_row, group_width, 0)
        partial_value = jnp.dot(left_part, right_part, preferred_element_type=jnp.float32)
        return (running + round_trip(partial_value), None)
    running = jnp.zeros((left.shape[0], right.shape[1]), jnp.float32)
    running, unused = lax.scan(add_group, running, jnp.arange(groups, dtype=jnp.int32))
    return running

def channel_mixer(normed, up_weight, down_weight, groups):
    group_width = up_weight.shape[1] // groups

    def add_group(running, number):
        first_row = (number * group_width).astype(jnp.int32)
        up_part = lax.dynamic_slice_in_dim(up_weight, first_row, group_width, 1)
        down_part = lax.dynamic_slice_in_dim(down_weight, first_row, group_width, 0)
        preact = jnp.maximum(jnp.dot(normed, up_part, preferred_element_type=jnp.float32), 0.0)
        hidden = (preact * preact).astype(jnp.bfloat16)
        partial_value = jnp.dot(hidden, down_part, preferred_element_type=jnp.float32)
        return (running + round_trip(partial_value), None)
    running = jnp.zeros((normed.shape[0], down_weight.shape[1]), jnp.float32)
    running, unused = lax.scan(add_group, running, jnp.arange(groups, dtype=jnp.int32))
    return running

def reference(resid, queries, keys, values, gates, log_decay, retention_output_weight, norm_gain, up_weight, down_weight):
    length = queries.shape[0]
    blocks = length // BLOCK
    token_indices = jnp.arange(length, dtype=jnp.int32)
    query_rot = round_trip(rotate(queries.astype(jnp.float32).reshape(length, HEADS, DK), token_indices))
    key_rot = round_trip(rotate(keys.astype(jnp.float32).reshape(length, HEADS, DK), token_indices) * DK ** (-0.5))
    cumulative = jnp.cumsum(log_decay.astype(jnp.float32).reshape(HEADS, blocks, BLOCK), axis=2)
    per_block = (query_rot.reshape(blocks, BLOCK, HEADS, DK), key_rot.reshape(blocks, BLOCK, HEADS, DK), values.astype(jnp.float32).reshape(blocks, BLOCK, HEADS, DV), gates.astype(jnp.float32).reshape(blocks, BLOCK, HEADS, DV), jnp.moveaxis(cumulative, 1, 0))
    unused, gated_out = lax.scan(block_step, jnp.zeros((HEADS, DK, DV), jnp.float32), per_block)
    gated_out = gated_out.reshape(length, HEADS * DV)
    mixed_sum = grouped_product(gated_out, retention_output_weight, N_TP)
    updated = (resid.astype(jnp.float32) + mixed_sum).astype(jnp.bfloat16)
    normed = normalize(updated, norm_gain)
    channel_sum = channel_mixer(normed, up_weight, down_weight, N_TP)
    return (updated.astype(jnp.float32) + channel_sum).astype(jnp.bfloat16)
```

```python
import functools

import jax
import jax.numpy as jnp
from jax import lax
from jax.experimental import pallas as pl
from jax.experimental.pallas import tpu as pltpu
from jax.sharding import PartitionSpec as P

DK = 256
DV = 512
BLOCK = 128
CORES = 2

tiny_stabilizer = 1e-06
F32 = jnp.float32
BF16 = jnp.bfloat16


def dot(a, b):
    return jnp.dot(a, b, preferred_element_type=F32)


def rotated(ref, cos_ref, sin_ref):
    x = ref[...].astype(F32)
    half = x.shape[1] // 2
    a, b = x[:, :half], x[:, half:]
    c, s = cos_ref[...], sin_ref[...]
    return jnp.concatenate([a * c - b * s, a * s + b * c], axis=1)


def cumulative(ld_ref):
    row = ld_ref[0, 0]
    n = row.shape[1]
    i = lax.broadcasted_iota(jnp.int32, (n, n), 0)
    j = lax.broadcasted_iota(jnp.int32, (n, n), 1)
    col = jnp.sum(jnp.where(i == j, row, 0.0), axis=1, keepdims=True)
    cum_col = jnp.sum(jnp.where(j <= i, row, 0.0), axis=1, keepdims=True)
    cum_row = jnp.sum(jnp.where(i <= j, col, 0.0), axis=0, keepdims=True)
    total = jnp.sum(row, axis=1, keepdims=True)
    return i, j, cum_col, cum_row, total


def block_term(key_rot, v_ref, cum_col, total):
    decayed = (key_rot.astype(F32) * jnp.exp(total - cum_col)).astype(BF16)
    return lax.dot_general(
        decayed, v_ref[...], (((0,), (0,)), ((), ())), preferred_element_type=F32
    )


def state_kernel(k_ref, v_ref, cos_ref, sin_ref, ld_ref, out_ref, st):
    b = pl.program_id(1)

    @pl.when(b == 0)
    def _():
        st[...] = jnp.zeros_like(st)

    i, j, cum_col, cum_row, total = cumulative(ld_ref)
    key_rot = (rotated(k_ref, cos_ref, sin_ref) * DK ** (-0.5)).astype(BF16)
    st[...] = jnp.exp(total) * st[...] + block_term(key_rot, v_ref, cum_col, total)

    @pl.when(b == pl.num_programs(1) - 1)
    def _():
        out_ref[0] = st[...].astype(BF16)


def local_kernel(q_ref, k_ref, v_ref, cos_ref, sin_ref, ld_ref, ret_ref, qdt_ref, st, run):
    b = pl.program_id(1)

    @pl.when(b == 0)
    def _():
        st[...] = jnp.zeros_like(st)
        run[...] = jnp.zeros_like(run)

    i, j, cum_col, cum_row, total = cumulative(ld_ref)
    key_rot = (rotated(k_ref, cos_ref, sin_ref) * DK ** (-0.5)).astype(BF16)
    query_rot = rotated(q_ref, cos_ref, sin_ref).astype(BF16)
    factor = jnp.where(i >= j, jnp.exp(jnp.minimum(cum_col - cum_row, 0.0)), 0.0)
    scores = lax.dot_general(
        query_rot, key_rot, (((1,), (1,)), ((), ())), preferred_element_type=F32
    )
    weights = (scores * factor).astype(BF16)
    q32 = query_rot.astype(F32)
    decayed = (q32 * jnp.exp(cum_col)).astype(BF16)
    ret_ref[...] = dot(weights, v_ref[...]) + dot(decayed, st[...].astype(BF16))
    before = run[:, 0:1]
    qdt_ref[...] = (q32 * jnp.exp(cum_col + before)).astype(BF16)
    run[...] = run[...] + total
    st[...] = jnp.exp(total) * st[...] + block_term(key_rot, v_ref, cum_col, total)


def finish_kernel(ret_ref, qdt_ref, inc_ref, gate_ref, out_ref):
    ret = ret_ref[...] + dot(qdt_ref[...], inc_ref[0])
    normed = ret * lax.rsqrt(jnp.mean(ret * ret, axis=1, keepdims=True) + tiny_stabilizer)
    out_ref[...] = (jax.nn.silu(gate_ref[...].astype(F32)) * normed).astype(BF16)


def params(n):
    return pltpu.CompilerParams(dimension_semantics=("arbitrary",) * n)


def cost(flops, size):
    return pl.CostEstimate(flops=flops, bytes_accessed=size, transcendentals=0)


def retention_state(keys, values, cos, sin, ld):
    heads, blocks = ld.shape[:2]
    return pl.pallas_call(
        state_kernel,
        grid=(heads, blocks),
        in_specs=[
            pl.BlockSpec((BLOCK, DK), lambda h, b: (b, h)),
            pl.BlockSpec((BLOCK, DV), lambda h, b: (b, h)),
            pl.BlockSpec((BLOCK, DK // 2), lambda h, b: (b, 0)),
            pl.BlockSpec((BLOCK, DK // 2), lambda h, b: (b, 0)),
            pl.BlockSpec((1, 1, 1, BLOCK), lambda h, b: (h, b, 0, 0)),
        ],
        out_specs=pl.BlockSpec((1, DK, DV), lambda h, b: (h, 0, 0)),
        out_shape=jax.ShapeDtypeStruct((heads, DK, DV), BF16),
        scratch_shapes=[pltpu.VMEM((DK, DV), F32)],
        compiler_params=params(2),
        cost_estimate=cost(4 * 10**9, 4 * 2**20),
    )(keys, values, cos, sin, ld)


def retention_local(queries, keys, values, cos, sin, ld):
    heads, blocks = ld.shape[:2]
    rows = queries.shape[0]
    at = lambda h, b: (b, h)
    return pl.pallas_call(
        local_kernel,
        grid=(heads, blocks),
        in_specs=[
            pl.BlockSpec((BLOCK, DK), at),
            pl.BlockSpec((BLOCK, DK), at),
            pl.BlockSpec((BLOCK, DV), at),
            pl.BlockSpec((BLOCK, DK // 2), lambda h, b: (b, 0)),
            pl.BlockSpec((BLOCK, DK // 2), lambda h, b: (b, 0)),
            pl.BlockSpec((1, 1, 1, BLOCK), lambda h, b: (h, b, 0, 0)),
        ],
        out_specs=[pl.BlockSpec((BLOCK, DV), at), pl.BlockSpec((BLOCK, DK), at)],
        out_shape=[
            jax.ShapeDtypeStruct((rows, heads * DV), F32),
            jax.ShapeDtypeStruct((rows, heads * DK), BF16),
        ],
        scratch_shapes=[pltpu.VMEM((DK, DV), F32), pltpu.VMEM((1, BLOCK), F32)],
        compiler_params=params(2),
        cost_estimate=cost(10 * 10**9, 10 * 2**20),
    )(queries, keys, values, cos, sin, ld)


def retention_finish(ret, qdt, incoming, gates):
    heads = incoming.shape[0]
    rows = ret.shape[0]
    tile = 256
    at = lambda h, r: (r, h)
    return pl.pallas_call(
        finish_kernel,
        grid=(heads, rows // tile),
        in_specs=[
            pl.BlockSpec((tile, DV), at),
            pl.BlockSpec((tile, DK), at),
            pl.BlockSpec((1, DK, DV), lambda h, r: (h, 0, 0)),
            pl.BlockSpec((tile, DV), at),
        ],
        out_specs=pl.BlockSpec((tile, DV), at),
        out_shape=jax.ShapeDtypeStruct((rows, heads * DV), BF16),
        compiler_params=params(2),
        cost_estimate=cost(3 * 10**9, 10 * 2**20),
    )(ret, qdt, incoming, gates)


def prefix_state(state, log_total, n):
    decay_in = jnp.exp(log_total)
    decays = []
    window, window_ex = decay_in, jnp.ones_like(decay_in)
    step = 1
    while step < n:
        pairs = [(k, k + step) for k in range(n - step)]
        got = lax.ppermute(window, "sp", pairs)
        decays.append((window, window_ex))
        window_ex = window_ex * got
        window = window * got
        step *= 2
    inclusive = state.astype(F32)
    exclusive = jnp.zeros_like(inclusive)
    sent = state
    step = 1
    for own, own_ex in decays:
        pairs = [(k, k + step) for k in range(n - step)]
        got = lax.ppermute(sent, "sp", pairs).astype(F32)
        exclusive = exclusive + own_ex[:, None, None] * got
        step *= 2
        if step < n:
            inclusive = inclusive + own[:, None, None] * got
            sent = inclusive.astype(BF16)
    return exclusive.astype(BF16)


def ring_pieces(piece, forward_steps, n):
    order = list(range(0, n, 2)) + list(range(n - 1, 0, -2))
    ahead = [(order[r], order[(r + 1) % n]) for r in range(n)]
    back = [(b, a) for a, b in ahead]
    pieces, offsets = [piece], [0]
    fwd = bwd = piece
    for s in range(1, n):
        if s <= forward_steps:
            fwd = lax.ppermute(fwd, "sp", ahead)
            pieces.append(fwd)
            offsets.append(-s)
        if s <= n - 1 - forward_steps:
            bwd = lax.ppermute(bwd, "sp", back)
            pieces.append(bwd)
            offsets.append(s)
    return pieces, offsets


def owners(offsets, n):
    me = lax.axis_index("sp")
    place = jnp.where(me % 2 == 0, me // 2, n - 1 - me // 2)
    out = []
    for o in offsets:
        r = (place + o + n) % n
        out.append(jnp.where(r < n // 2, 2 * r, 2 * (n - 1 - r) + 1))
    return jnp.stack(out).astype(jnp.int32)


def mixer_kernel(n, up_owner, down_owner, x_ref, *refs):
    ups, downs = refs[:n], refs[n : 2 * n]
    out_ref, up_all, acc = refs[2 * n :]
    f = pl.program_id(0)
    rows_up = ups[0].shape[0]
    cols = downs[0].shape[1]
    for k in range(n):
        up_all[pl.ds(pl.multiple_of(up_owner[k] * rows_up, rows_up), rows_up), :] = ups[k][...]
    preact = jnp.maximum(dot(x_ref[...], up_all[...]), 0.0)
    hidden = (preact * preact).astype(BF16)
    last = pl.num_programs(0) - 1
    for k in range(n):
        at = pl.ds(pl.multiple_of(down_owner[k] * cols, cols), cols)
        part = dot(hidden, downs[k][...])

        @pl.when(f == 0)
        def _():
            acc[:, at] = part

        @pl.when(f > 0)
        def _():
            acc[:, at] += part

    @pl.when(f == last)
    def _():
        out_ref[...] = acc[...].astype(BF16)


def mixer(x, ups, downs, up_owner, down_owner):
    n = len(ups)
    m, d = x.shape
    ff = ups[0].shape[1]
    tile = min(512, ff)
    return pl.pallas_call(
        functools.partial(mixer_kernel, n),
        grid_spec=pltpu.PrefetchScalarGridSpec(
            num_scalar_prefetch=2,
            grid=(ff // tile,),
            in_specs=[pl.BlockSpec((m, d), lambda f, *_: (0, 0))]
            + [pl.BlockSpec((d // n, tile), lambda f, *_: (0, f))] * n
            + [pl.BlockSpec((tile, d // n), lambda f, *_: (f, 0))] * n,
            out_specs=pl.BlockSpec((m, d), lambda f, *_: (0, 0)),
            scratch_shapes=[pltpu.VMEM((d, tile), BF16), pltpu.VMEM((m, d), F32)],
        ),
        out_shape=jax.ShapeDtypeStruct((m, d), BF16),
        compiler_params=params(1),
        cost_estimate=cost(4 * m * d * ff, 20 * 2**20),
    )(up_owner, down_owner, x, *ups, *downs)


def normalize(updated, norm_gain):
    widened = updated.astype(F32)
    scaled = widened * lax.rsqrt(
        jnp.mean(widened * widened, axis=-1, keepdims=True) + tiny_stabilizer
    )
    return (scaled * norm_gain.astype(F32)).astype(BF16)


def body(n_sp, n_tp, resid, queries, keys, values, gates, log_decay, w_out, gain, up, down):
    chips = n_tp // CORES
    t = lax.axis_index("tp")
    x, core = t // CORES, t % CORES
    swap = [(k, k ^ 1) for k in range(n_tp)]

    def to_chip(s):
        return [(k, (k + CORES * s) % n_tp) for k in range(n_tp)]

    half = n_sp // 2
    ups, up_off = ring_pieces(up, half, n_sp)
    downs, down_off = ring_pieces(down, n_sp - 1 - half, n_sp)

    rows = queries.shape[0]
    heads = log_decay.shape[0]
    blocks = rows // BLOCK
    where = (lax.axis_index("sp") * rows + jnp.arange(rows, dtype=jnp.int32)).astype(F32)
    inverse = 10000.0 ** (-jnp.arange(0, DK, 2, dtype=F32) / DK)
    angles = where[:, None] * inverse[None, :]
    cos, sin = jnp.cos(angles), jnp.sin(angles)
    ld = log_decay.reshape(heads, blocks, 1, BLOCK)
    state = retention_state(keys, values, cos, sin, ld)
    incoming = prefix_state(state, jnp.sum(log_decay, axis=1), n_sp)
    ret, qdt = retention_local(queries, keys, values, cos, sin, ld)
    gated = retention_finish(ret, qdt, incoming, gates)

    mine = rows // n_tp
    grouped = gated.reshape(chips, CORES, mine, gated.shape[1])

    def reduce_to_owner(parts):
        total = None
        for s in list(range(1, chips)) + [0]:
            same, other = parts(s)
            got = lax.ppermute(other, "tp", swap)
            both = same.astype(F32) + got.astype(F32)
            if s:
                both = lax.ppermute(both.astype(BF16), "tp", to_chip(s)).astype(F32)
            total = both if total is None else total + both
        return total

    def projected(s):
        chip = lax.dynamic_index_in_dim(grouped, (x + s) % chips, 0, keepdims=False)
        same = lax.dynamic_index_in_dim(chip, core, 0, keepdims=False)
        other = lax.dynamic_index_in_dim(chip, 1 - core, 0, keepdims=False)
        return dot(same, w_out).astype(BF16), dot(other, w_out).astype(BF16)

    updated = (resid.astype(F32) + reduce_to_owner(projected)).astype(BF16)
    normed = normalize(updated, gain)

    up_owner, down_owner = owners(up_off, n_sp), owners(down_off, n_sp)
    sources = {0: normed}
    for s in range(1, chips):
        sources[s] = lax.ppermute(normed, "tp", to_chip(chips - s))

    def mixed(s):
        other = lax.ppermute(sources[s], "tp", swap)
        both = jnp.concatenate([sources[s], other], axis=0)
        out = mixer(both, ups, downs, up_owner, down_owner)
        return out[:mine], out[mine:]

    near = mixed(0)

    def channel(s):
        return mixed(s) if s else near

    return (updated.astype(F32) + reduce_to_owner(channel)).astype(BF16)


def solution(mesh):
    placed = (
        P(("sp", "tp"), None),
        P("sp", "tp"),
        P("sp", "tp"),
        P("sp", "tp"),
        P("sp", "tp"),
        P("tp", "sp"),
        P("tp", None),
        P(),
        P("sp", "tp"),
        P("tp", "sp"),
    )
    return jax.shard_map(
        functools.partial(body, mesh.shape["sp"], mesh.shape["tp"]),
        mesh=mesh,
        in_specs=placed,
        out_specs=P(("sp", "tp"), None),
        check_vma=False,
    )
```

```python
import functools

import jax
import jax.numpy as jnp
from jax import lax
from jax.experimental import pallas as pl
from jax.experimental.pallas import tpu as pltpu
from jax.sharding import PartitionSpec as P

DK = 256
DV = 512
BLOCK = 128
CORES = 2

tiny_stabilizer = 1e-06
F32 = jnp.float32
BF16 = jnp.bfloat16


def dot(a, b):
    return jnp.dot(a, b, preferred_element_type=F32)


def rotated(ref, cos_ref, sin_ref):
    x = ref[...].astype(F32)
    half = x.shape[1] // 2
    a, b = x[:, :half], x[:, half:]
    c, s = cos_ref[...], sin_ref[...]
    return jnp.concatenate([a * c - b * s, a * s + b * c], axis=1)


def cumulative(ld_ref):
    row = ld_ref[0, 0]
    n = row.shape[1]
    i = lax.broadcasted_iota(jnp.int32, (n, n), 0)
    j = lax.broadcasted_iota(jnp.int32, (n, n), 1)
    col = jnp.sum(jnp.where(i == j, row, 0.0), axis=1, keepdims=True)
    cum_col = jnp.sum(jnp.where(j <= i, row, 0.0), axis=1, keepdims=True)
    cum_row = jnp.sum(jnp.where(i <= j, col, 0.0), axis=0, keepdims=True)
    total = jnp.sum(row, axis=1, keepdims=True)
    return i, j, cum_col, cum_row, total


def block_term(key_rot, v_ref, cum_col, total):
    decayed = (key_rot.astype(F32) * jnp.exp(total - cum_col)).astype(BF16)
    return lax.dot_general(
        decayed, v_ref[...], (((0,), (0,)), ((), ())), preferred_element_type=F32
    )


def state_kernel(k_ref, v_ref, cos_ref, sin_ref, ld_ref, out_ref, st):
    b = pl.program_id(1)

    @pl.when(b == 0)
    def _():
        st[...] = jnp.zeros_like(st)

    _, _, cum_col, _, total = cumulative(ld_ref)
    key_rot = (rotated(k_ref, cos_ref, sin_ref) * DK ** (-0.5)).astype(BF16)
    st[...] = jnp.exp(total) * st[...] + block_term(key_rot, v_ref, cum_col, total)

    @pl.when(b == pl.num_programs(1) - 1)
    def _():
        out_ref[0] = st[...].astype(BF16)


def local_kernel(q_ref, k_ref, v_ref, cos_ref, sin_ref, ld_ref, ret_ref, qdt_ref, st, run):
    b = pl.program_id(1)

    @pl.when(b == 0)
    def _():
        st[...] = jnp.zeros_like(st)
        run[...] = jnp.zeros_like(run)

    i, j, cum_col, cum_row, total = cumulative(ld_ref)
    key_rot = (rotated(k_ref, cos_ref, sin_ref) * DK ** (-0.5)).astype(BF16)
    query_rot = rotated(q_ref, cos_ref, sin_ref).astype(BF16)
    factor = jnp.where(i >= j, jnp.exp(jnp.minimum(cum_col - cum_row, 0.0)), 0.0)
    scores = lax.dot_general(
        query_rot, key_rot, (((1,), (1,)), ((), ())), preferred_element_type=F32
    )
    weights = (scores * factor).astype(BF16)
    q32 = query_rot.astype(F32)
    decayed = (q32 * jnp.exp(cum_col)).astype(BF16)
    ret_ref[...] = dot(weights, v_ref[...]) + dot(decayed, st[...].astype(BF16))
    before = run[:, 0:1]
    qdt_ref[...] = (q32 * jnp.exp(cum_col + before)).astype(BF16)
    run[...] = run[...] + total
    st[...] = jnp.exp(total) * st[...] + block_term(key_rot, v_ref, cum_col, total)


def finish_kernel(place, ret_ref, qdt_ref, inc_ref, gate_ref, out_ref):
    ret = ret_ref[...] + dot(qdt_ref[...], inc_ref[0])
    normed = ret * lax.rsqrt(jnp.mean(ret * ret, axis=1, keepdims=True) + tiny_stabilizer)
    out_ref[...] = (jax.nn.silu(gate_ref[...].astype(F32)) * normed).astype(BF16)


def params(n):
    return pltpu.CompilerParams(dimension_semantics=("arbitrary",) * n)


def cost(flops, size):
    return pl.CostEstimate(flops=flops, bytes_accessed=size, transcendentals=0)


def retention_state(keys, values, cos, sin, ld):
    heads, blocks = ld.shape[:2]
    return pl.pallas_call(
        state_kernel,
        grid=(heads, blocks),
        in_specs=[
            pl.BlockSpec((BLOCK, DK), lambda h, b: (b, h)),
            pl.BlockSpec((BLOCK, DV), lambda h, b: (b, h)),
            pl.BlockSpec((BLOCK, DK // 2), lambda h, b: (b, 0)),
            pl.BlockSpec((BLOCK, DK // 2), lambda h, b: (b, 0)),
            pl.BlockSpec((1, 1, 1, BLOCK), lambda h, b: (h, b, 0, 0)),
        ],
        out_specs=pl.BlockSpec((1, DK, DV), lambda h, b: (h, 0, 0)),
        out_shape=jax.ShapeDtypeStruct((heads, DK, DV), BF16),
        scratch_shapes=[pltpu.VMEM((DK, DV), F32)],
        compiler_params=params(2),
        cost_estimate=cost(4 * 10**9, 4 * 2**20),
    )(keys, values, cos, sin, ld)


def retention_local(queries, keys, values, cos, sin, ld):
    heads, blocks = ld.shape[:2]
    rows = queries.shape[0]
    at = lambda h, b: (b, h)
    return pl.pallas_call(
        local_kernel,
        grid=(heads, blocks),
        in_specs=[
            pl.BlockSpec((BLOCK, DK), at),
            pl.BlockSpec((BLOCK, DK), at),
            pl.BlockSpec((BLOCK, DV), at),
            pl.BlockSpec((BLOCK, DK // 2), lambda h, b: (b, 0)),
            pl.BlockSpec((BLOCK, DK // 2), lambda h, b: (b, 0)),
            pl.BlockSpec((1, 1, 1, BLOCK), lambda h, b: (h, b, 0, 0)),
        ],
        out_specs=[pl.BlockSpec((BLOCK, DV), at), pl.BlockSpec((BLOCK, DK), at)],
        out_shape=[
            jax.ShapeDtypeStruct((rows, heads * DV), F32),
            jax.ShapeDtypeStruct((rows, heads * DK), BF16),
        ],
        scratch_shapes=[pltpu.VMEM((DK, DV), F32), pltpu.VMEM((1, BLOCK), F32)],
        compiler_params=params(2),
        cost_estimate=cost(10 * 10**9, 10 * 2**20),
    )(queries, keys, values, cos, sin, ld)


def retention_finish(place, ret, qdt, incoming, gates):
    heads = incoming.shape[0]
    rows = ret.shape[0]
    tile = rows // place.shape[0]
    at = lambda h, r, *_: (r, h)
    return pl.pallas_call(
        finish_kernel,
        grid_spec=pltpu.PrefetchScalarGridSpec(
            num_scalar_prefetch=1,
            grid=(heads, rows // tile),
            in_specs=[
                pl.BlockSpec((tile, DV), at),
                pl.BlockSpec((tile, DK), at),
                pl.BlockSpec((1, DK, DV), lambda h, r, *_: (h, 0, 0)),
                pl.BlockSpec((tile, DV), at),
            ],
            out_specs=pl.BlockSpec((tile, DV), lambda h, r, place: (place[r], h)),
        ),
        out_shape=jax.ShapeDtypeStruct((rows, heads * DV), BF16),
        compiler_params=params(2),
        cost_estimate=cost(3 * 10**9, 10 * 2**20),
    )(place, ret, qdt, incoming, gates)


def prefix_state(state, log_total, n):
    decay_in = jnp.exp(log_total)
    decays = []
    window, window_ex = decay_in, jnp.ones_like(decay_in)
    step = 1
    while step < n:
        pairs = [(k, k + step) for k in range(n - step)]
        got = lax.ppermute(window, "sp", pairs)
        decays.append((window, window_ex))
        window_ex = window_ex * got
        window = window * got
        step *= 2
    inclusive = state.astype(F32)
    exclusive = jnp.zeros_like(inclusive)
    sent = state
    step = 1
    for own, own_ex in decays:
        pairs = [(k, k + step) for k in range(n - step)]
        got = lax.ppermute(sent, "sp", pairs).astype(F32)
        exclusive = exclusive + own_ex[:, None, None] * got
        step *= 2
        if step < n:
            inclusive = inclusive + own[:, None, None] * got
            sent = inclusive.astype(BF16)
    return exclusive.astype(BF16)


def ring(n):
    order = list(range(0, n, 2)) + list(range(n - 1, 0, -2))
    ahead = [(order[r], order[(r + 1) % n]) for r in range(n)]
    return ahead, [(b, a) for a, b in ahead]


def ring_pieces(piece, forward_steps, n):
    ahead, back = ring(n)
    fwd = bwd = piece
    pieces, offsets = [piece], [0]
    for s in range(1, n):
        if s <= forward_steps:
            fwd = lax.ppermute(fwd, "sp", ahead)
            pieces.append(fwd)
            offsets.append(-s)
        if s <= n - 1 - forward_steps:
            bwd = lax.ppermute(bwd, "sp", back)
            pieces.append(bwd)
            offsets.append(s)
    return pieces, offsets


def owners(offsets, n):
    me = lax.axis_index("sp")
    place = jnp.where(me % 2 == 0, me // 2, n - 1 - me // 2)
    out = []
    for o in offsets:
        r = (place + o + n) % n
        out.append(jnp.where(r < n // 2, 2 * r, 2 * (n - 1 - r) + 1))
    return jnp.stack(out).astype(jnp.int32)


def hidden_kernel(n, owner, other_ref, same_ref, *refs):
    ups, (out_ref, up_all) = refs[:n], refs[n:]
    rows_up = ups[0].shape[0]
    half = other_ref.shape[0]
    for k in range(n):
        up_all[pl.ds(pl.multiple_of(owner[k] * rows_up, rows_up), rows_up), :] = ups[k][...]
    for g, x_ref in enumerate((other_ref, same_ref)):
        preact = jnp.maximum(dot(x_ref[...], up_all[...]), 0.0)
        out_ref[g * half : (g + 1) * half, :] = (preact * preact).astype(BF16)


def hidden_of(other, same, ups, owner):
    n = len(ups)
    m, d = other.shape
    ff = ups[0].shape[1]
    tile = min(512, ff)
    return pl.pallas_call(
        functools.partial(hidden_kernel, n),
        grid_spec=pltpu.PrefetchScalarGridSpec(
            num_scalar_prefetch=1,
            grid=(ff // tile,),
            in_specs=[pl.BlockSpec((m, d), lambda f, *_: (0, 0))] * 2
            + [pl.BlockSpec((d // n, tile), lambda f, *_: (0, f))] * n,
            out_specs=pl.BlockSpec((2 * m, tile), lambda f, *_: (0, f)),
            scratch_shapes=[pltpu.VMEM((d, tile), BF16)],
        ),
        out_shape=jax.ShapeDtypeStruct((2 * m, ff), BF16),
        compiler_params=params(1),
        cost_estimate=cost(4 * m * d * ff, 16 * 2**20),
    )(owner, other, same, *ups)


def down_kernel(n, h_ref, *refs):
    downs, (other_ref, same_ref) = refs[:n], refs[n:]
    i = pl.program_id(0)
    half = pl.num_programs(0) // 2
    cols = downs[0].shape[1]
    h = h_ref[...]

    @pl.when(i < half)
    def _():
        for k in range(n):
            other_ref[:, k * cols : (k + 1) * cols] = dot(h, downs[k][...]).astype(BF16)

    @pl.when(i >= half)
    def _():
        for k in range(n):
            same_ref[:, k * cols : (k + 1) * cols] = dot(h, downs[k][...]).astype(BF16)


def down_of(hidden, downs, tile):
    n = len(downs)
    m, ff = hidden.shape
    cols = downs[0].shape[1]
    steps = m // tile
    half = steps // 2
    shape = jax.ShapeDtypeStruct((m // 2, n * cols), BF16)
    return pl.pallas_call(
        functools.partial(down_kernel, n),
        grid=(steps,),
        in_specs=[pl.BlockSpec((tile, ff), lambda i: (i, 0))]
        + [pl.BlockSpec((ff, cols), lambda i: (0, 0))] * n,
        out_specs=[
            pl.BlockSpec((tile, n * cols), lambda i: (jnp.minimum(i, half - 1), 0)),
            pl.BlockSpec((tile, n * cols), lambda i: (jnp.maximum(i - half, 0), 0)),
        ],
        out_shape=[shape, shape],
        compiler_params=params(1),
        cost_estimate=cost(2 * m * n * cols * ff, 10 * 2**20),
    )(hidden, *downs)


def close_kernel(owner, upd_ref, *refs):
    sums, out_ref = refs[:-1], refs[-1]
    cols = upd_ref.shape[1] // owner.shape[0]
    done = 0
    for sum_ref in sums:
        for k in range(sum_ref.shape[1] // cols):
            at = pl.ds(pl.multiple_of(owner[done] * cols, cols), cols)
            part = sum_ref[:, k * cols : (k + 1) * cols]
            out_ref[:, at] = (upd_ref[:, at].astype(F32) + part).astype(BF16)
            done += 1


def close(owner, updated, sums):
    m, d = updated.shape
    tile = m // 4
    at = lambda r, *_: (r, 0)
    return pl.pallas_call(
        close_kernel,
        grid_spec=pltpu.PrefetchScalarGridSpec(
            num_scalar_prefetch=1,
            grid=(4,),
            in_specs=[pl.BlockSpec((tile, a.shape[1]), at) for a in (updated, *sums)],
            out_specs=pl.BlockSpec((tile, d), at),
        ),
        out_shape=jax.ShapeDtypeStruct((m, d), BF16),
        compiler_params=params(1),
        cost_estimate=cost(m * d, 4 * 2**20),
    )(owner, updated, *sums)


def normalize(updated, norm_gain):
    widened = updated.astype(F32)
    scaled = widened * lax.rsqrt(
        jnp.mean(widened * widened, axis=-1, keepdims=True) + tiny_stabilizer
    )
    return (scaled * norm_gain.astype(F32)).astype(BF16)


def body(n_sp, n_tp, resid, queries, keys, values, gates, log_decay, w_out, gain, up, down):
    chips = n_tp // CORES
    t = lax.axis_index("tp")
    x, core = t // CORES, t % CORES
    swap = [(k, k ^ 1) for k in range(n_tp)]

    def to_chip(s):
        return [(k, (k + CORES * s) % n_tp) for k in range(n_tp)]

    half = n_sp // 2
    ups, up_off = ring_pieces(up, half, n_sp)
    downs, down_off = ring_pieces(down, n_sp - 1 - half, n_sp)
    up_owner, down_owner = owners(up_off, n_sp), owners(down_off, n_sp)

    rows = queries.shape[0]
    heads = log_decay.shape[0]
    blocks = rows // BLOCK
    mine = rows // n_tp
    where = (lax.axis_index("sp") * rows + jnp.arange(rows, dtype=jnp.int32)).astype(F32)
    inverse = 10000.0 ** (-jnp.arange(0, DK, 2, dtype=F32) / DK)
    angles = where[:, None] * inverse[None, :]
    cos, sin = jnp.cos(angles), jnp.sin(angles)
    ld = log_decay.reshape(heads, blocks, 1, BLOCK)
    state = retention_state(keys, values, cos, sin, ld)
    incoming = prefix_state(state, jnp.sum(log_decay, axis=1), n_sp)
    ret, qdt = retention_local(queries, keys, values, cos, sin, ld)
    tile = jnp.arange(n_tp, dtype=jnp.int32)
    place = (tile // CORES - x + 2 * chips - 1) % chips
    place = place + jnp.where(tile % CORES == core, chips, 0)
    gated = retention_finish(place.astype(jnp.int32), ret, qdt, incoming, gates)

    def reduce_to_owner(other, same):
        got = lax.ppermute(other, "tp", swap)
        both = (same.astype(F32) + got.astype(F32)).reshape(chips, mine, same.shape[1])
        total = both[chips - 1]
        for s in range(1, chips):
            sent = lax.ppermute(both[s - 1].astype(BF16), "tp", to_chip(s))
            total = total + sent.astype(F32)
        return total

    other = dot(gated[: rows // 2], w_out).astype(BF16)
    same = dot(gated[rows // 2 :], w_out).astype(BF16)
    updated = (resid.astype(F32) + reduce_to_owner(other, same)).astype(BF16)
    normed = normalize(updated, gain)

    same = [lax.ppermute(normed, "tp", to_chip(chips - s)) for s in range(1, chips)]
    same = jnp.concatenate(same + [normed], axis=0)
    other = lax.ppermute(same, "tp", swap)
    hidden = hidden_of(other, same, ups, up_owner)
    cut = max(1, n_sp - 3)
    sums = []
    for group in (downs[:cut], downs[cut:]):
        out_other, out_same = down_of(hidden, group, mine)
        sums.append(reduce_to_owner(out_other, out_same))
    return close(down_owner, updated, sums)


def solution(mesh):
    placed = (
        P(("sp", "tp"), None),
        P("sp", "tp"),
        P("sp", "tp"),
        P("sp", "tp"),
        P("sp", "tp"),
        P("tp", "sp"),
        P("tp", None),
        P(),
        P("sp", "tp"),
        P("tp", "sp"),
    )
    return jax.shard_map(
        functools.partial(body, mesh.shape["sp"], mesh.shape["tp"]),
        mesh=mesh,
        in_specs=placed,
        out_specs=P(("sp", "tp"), None),
        check_vma=False,
    )
```
